32 devices in a mesh: rep: 2 (over x), fs: 8 (over z, y), tp: 2 (over core).
Axes of the slice: x: 2, y: 2, z: 4, core: 2. Of those that a mesh axis runs over, the one named last changes fastest.
Arguments:
- inputs: bfloat16 [2048, 2048], P(('rep', 'fs'), 'tp'), may hold values from -6 to 6
- cotangent: bfloat16 [2048, 2048], P(('rep', 'fs'), 'tp'), may hold values from -8 to 8
- gate_weight: bfloat16 [2048, 2816], P('fs', 'tp'), may hold values from -0.125 to 0.125
- up_weight: bfloat16 [2048, 2816], P('fs', 'tp'), may hold values from -0.125 to 0.125
- down_weight: bfloat16 [2816, 2048], P('tp', 'fs'), may hold values from -0.109375 to 0.109375
Outputs:
- grad_inputs: bfloat16 [2048, 2048], P(('rep', 'fs'), 'tp')
- grad_gate_weight: float32 [2048, 2816], P('fs', 'tp')
- grad_up_weight: float32 [2048, 2816], P('fs', 'tp')
- grad_down_weight: float32 [2816, 2048], P('tp', 'fs')
The draws below stay inside these ranges and needn't reach their ends.
All inputs are finite; a program needn't handle non-finite values.
Results may differ from the reference program's by a relative error of at most 0.014.
Values may be sent and summed in bfloat16 or wider, within the bound.
A program may use at most 64 MiB of HBM per device.

```python
import jax
import jax.numpy as jnp
from jax import lax

D = 2048
FF = 2816
TOKENS = 2048
N_TP = 2


def strengthened(result, rng, source, target, blocks, factor):
    def block_of(position):
        return (jnp.arange(result.shape[position]) // (result.shape[position] // blocks)).reshape((-1,) + (1,) * (result.ndim - 1 - position))

    one_side = jax.random.permutation(rng, blocks)[block_of(target)]
    other_side = (block_of(target) + blocks // 2) % blocks
    return jnp.where((block_of(source) == one_side) | (block_of(source) == other_side), factor * result, result)


def block_scale(rng, shape, split, least, top_value):
    def one(axis_at, shards_of):
        steps = jax.random.uniform(jax.random.fold_in(jax.random.fold_in(rng, 6), axis_at), (shards_of,), jnp.float32, least / len(split), top_value / len(split))
        return jnp.repeat(jnp.exp(steps), shape[axis_at] // shards_of).reshape((-1,) + (1,) * (len(shape) - axis_at - 1))

    loudness = one(*split[0])
    for cut in split[1:]:
        loudness = loudness * one(*cut)
    return loudness


def noise(stream_key, extent, deviation, reach, shards=(), kind=jnp.bfloat16):
    drawn = deviation * jax.random.normal(stream_key, extent, jnp.float32)
    if shards:
        drawn = drawn * block_scale(stream_key, extent, shards, -0.22, 0.18)
    return jnp.clip(drawn, -reach, reach).astype(kind)


def gaussian_with(own_key, extent, spread, bound, shards, heavy, held_as=jnp.bfloat16):
    drawn = spread * jax.random.normal(own_key, extent, jnp.float32)
    if shards:
        drawn = drawn * block_scale(own_key, extent, shards, -0.22, 0.18)
    return jnp.clip(strengthened(drawn, jax.random.fold_in(own_key, 3), *heavy), -bound, bound).astype(held_as)


def setup_inputs(seed: int = 0) -> dict:
    streams_of = jax.random.split(jax.random.key(seed), 6)
    return {
        "inputs": noise(streams_of[0], (TOKENS, D), 1.0, 6.0, ((0, 16), (1, 2))),
        "cotangent": gaussian_with(streams_of[1], (TOKENS, D), 1.0, 8.0, ((0, 16), (1, 2)), (0, 1, 16, 2.0)),
        "gate_weight": noise(streams_of[2], (D, FF), D ** -0.5, 0.125, ((0, 8), (1, 2))),
        "up_weight": noise(streams_of[3], (D, FF), D ** -0.5, 0.125, ((0, 8), (1, 2))),
        "down_weight": noise(streams_of[4], (FF, D), FF ** -0.5, 0.109375, ((0, 2), (1, 8))),
    }


def reference(inputs, cotangent, gate_weight, up_weight, down_weight):
    gate_pre = jnp.dot(inputs, gate_weight, preferred_element_type=jnp.float32)
    up_pre = jnp.dot(inputs, up_weight, preferred_element_type=jnp.float32)
    sigmoid_gate = jax.nn.sigmoid(gate_pre)
    activated = gate_pre * sigmoid_gate
    hidden = (activated * up_pre).astype(jnp.bfloat16)
    grad_hidden = jnp.dot(cotangent, down_weight.T, preferred_element_type=jnp.float32)
    grad_gate = (grad_hidden * up_pre * sigmoid_gate * (1.0 + gate_pre * (1.0 - sigmoid_gate))).astype(jnp.bfloat16)
    grad_up = (grad_hidden * activated).astype(jnp.bfloat16)
    grad_down_weight = jnp.dot(hidden.T, cotangent, preferred_element_type=jnp.float32)
    grad_gate_weight = jnp.dot(inputs.T, grad_gate, preferred_element_type=jnp.float32)
    grad_up_weight = jnp.dot(inputs.T, grad_up, preferred_element_type=jnp.float32)
    block_units = FF // N_TP
    running = jnp.zeros(inputs.shape, jnp.float32)
    for index in range(N_TP):
        lower = index * block_units
        upper = lower + block_units
        partial_sum = jnp.dot(grad_gate[:, lower:upper], gate_weight[:, lower:upper].T, preferred_element_type=jnp.float32)
        partial_sum = partial_sum + jnp.dot(grad_up[:, lower:upper], up_weight[:, lower:upper].T, preferred_element_type=jnp.float32)
        rounded = lax.optimization_barrier(partial_sum.astype(jnp.bfloat16))
        running = running + rounded.astype(jnp.float32)
    grad_inputs = running.astype(jnp.bfloat16)
    return (grad_inputs, grad_gate_weight, grad_up_weight, grad_down_weight)
```

```python
import functools

import jax
import jax.numpy as jnp
from jax import lax
from jax.experimental import pallas as pl
from jax.experimental.pallas import tpu as pltpu
from jax.sharding import PartitionSpec as P

MESH = pl.DeviceIdType.MESH


def enter(n_rep, n_fs, n_tp):
    barrier = pltpu.get_barrier_semaphore()
    for axis, n in (("rep", n_rep), ("fs", n_fs), ("tp", n_tp)):
        me = lax.axis_index(axis)
        for k in range(1, n):
            pl.semaphore_signal(
                barrier, inc=1, device_id={axis: lax.rem(me + k, n)}, device_id_type=MESH
            )
    pl.semaphore_wait(barrier, n_rep + n_fs + n_tp - 3)


class Sender:
    def __init__(self, sems):
        self.sems, self.used, self.pending = sems, 0, []

    def send(self, src, dst, recv_sem, axis, peer):
        copy = pltpu.make_async_remote_copy(
            src_ref=src,
            dst_ref=dst,
            send_sem=self.sems.at[self.used],
            recv_sem=recv_sem,
            device_id={axis: peer},
            device_id_type=MESH,
        )
        self.used += 1
        copy.start()
        self.pending.append(copy)

    def local(self, src, dst):
        copy = pltpu.make_async_copy(src, dst, self.sems.at[self.used])
        self.used += 1
        copy.start()
        self.pending.append(copy)

    def finish(self):
        for copy in self.pending:
            if hasattr(copy, "wait_send") and copy.is_remote:
                copy.wait_send()
            else:
                copy.wait()


def arrived(slot, recv_sem):
    pltpu.make_async_copy(slot, slot, recv_sem).wait()


def near_first(n):
    return sorted(range(1, n), key=lambda k: min(k, n - k))


def gather_kernel(
    sizes, x_ref, c_ref, w_ref, x_out, c_out, w_out, sends, act_recv, w_recv
):
    n_rep, n_fs, n_tp, n_y = sizes
    n_z = n_fs // n_y
    rep, fs, tp = (lax.axis_index(axis) for axis in ("rep", "fs", "tp"))
    z, y = fs // n_y, lax.rem(fs, n_y)
    width = x_ref.shape[1]
    depth = w_ref.shape[3]
    enter(n_rep, n_fs, n_tp)
    out = Sender(sends)
    acts = ((x_ref, x_out), (c_ref, c_out))

    def act_slot(a, owner, part):
        return acts[a][1].at[owner, :, pl.ds(pl.multiple_of(part * width, width), width)]

    def w_slot(half, owner):
        if depth % 128 == 0:
            return w_out.at[half, :, pl.ds(pl.multiple_of(owner * depth, depth), depth)]
        return w_out.at[half, owner]

    def to_tp(a, owner, src):
        for k in range(1, n_tp):
            out.send(
                src, act_slot(a, owner, tp), act_recv.at[a, owner, tp], "tp", lax.rem(tp + k, n_tp)
            )

    def to_y(a, owner, src):
        for k in range(1, n_y):
            peer = z * n_y + lax.rem(y + k, n_y)
            out.send(src, act_slot(a, owner, tp), act_recv.at[a, owner, tp], "fs", peer)

    for a in range(2):
        src = acts[a][0]
        to_y(a, fs, src)
        for k in near_first(n_z):
            peer = lax.rem(z + k, n_z) * n_y + y
            out.send(src, act_slot(a, fs, tp), act_recv.at[a, fs, tp], "fs", peer)
    for k in near_first(n_fs):
        peer = lax.rem(fs + k, n_fs)
        out.send(w_ref.at[peer, rep], w_slot(rep, fs), w_recv.at[rep, fs], "fs", peer)
    for k in range(1, n_rep):
        out.send(
            w_ref.at[fs, rep], w_slot(rep, fs), w_recv.at[rep, fs], "rep", lax.rem(rep + k, n_rep)
        )
    for a in range(2):
        to_tp(a, fs, acts[a][0])
        out.local(acts[a][0], act_slot(a, fs, tp))
    out.local(w_ref.at[fs, rep], w_slot(rep, fs))

    for k in near_first(n_z):
        owner = lax.rem(z + n_z - k, n_z) * n_y + y
        for a in range(2):
            slot = act_slot(a, owner, tp)
            arrived(slot, act_recv.at[a, owner, tp])
            to_y(a, owner, slot)
            to_tp(a, owner, slot)
    for k in near_first(n_fs):
        owner = lax.rem(fs + n_fs - k, n_fs)
        slot = w_slot(rep, owner)
        arrived(slot, w_recv.at[rep, owner])
        for j in range(1, n_rep):
            out.send(slot, w_slot(rep, owner), w_recv.at[rep, owner], "rep", lax.rem(rep + j, n_rep))
    for kz in [0] + near_first(n_z):
        for ky in range(1, n_y):
            owner = lax.rem(z + n_z - kz, n_z) * n_y + lax.rem(y + ky, n_y)
            for a in range(2):
                slot = act_slot(a, owner, tp)
                arrived(slot, act_recv.at[a, owner, tp])
                to_tp(a, owner, slot)
    for j in range(1, n_rep):
        half = lax.rem(rep + j, n_rep)
        for k in range(n_fs):
            owner = lax.rem(fs + k, n_fs)
            arrived(w_slot(half, owner), w_recv.at[half, owner])
    for j in range(1, n_tp):
        part = lax.rem(tp + j, n_tp)
        for k in range(n_fs):
            owner = lax.rem(fs + k, n_fs)
            for a in range(2):
                arrived(act_slot(a, owner, part), act_recv.at[a, owner, part])
    out.finish()


def scatter_kernel(
    sizes, p_ref, g_ref, x_out, g_out,
    p_in, p_sum, g_in, g_sum, sends, p_recv, g_recv, x_recv, gx_recv,
):
    n_rep, n_fs, n_tp = sizes
    rep, fs, tp = (lax.axis_index(axis) for axis in ("rep", "fs", "tp"))
    rows, width = p_sum.shape[1:]
    enter(n_rep, n_fs, n_tp)
    out = Sender(sends)
    order = near_first(n_fs) + [0]

    def p_part(owner, part):
        return p_ref.at[owner, :, pl.ds(pl.multiple_of(part * width, width), width)]

    for k in order:
        owner = lax.rem(fs + k, n_fs)
        for j in range(1, n_tp):
            peer = lax.rem(tp + j, n_tp)
            out.send(p_part(owner, peer), p_in.at[j - 1, owner], p_recv.at[j - 1, owner], "tp", peer)
    for k in order:
        owner = lax.rem(fs + k, n_fs)
        for j in range(1, n_rep):
            peer = lax.rem(rep + j, n_rep)
            out.send(
                g_ref.at[owner, peer], g_in.at[j - 1, owner], g_recv.at[j - 1, owner], "rep", peer
            )
    for k in order:
        owner = lax.rem(fs + k, n_fs)
        total = p_part(owner, tp)[...].astype(jnp.float32)
        for j in range(n_tp - 1):
            arrived(p_in.at[j, owner], p_recv.at[j, owner])
            total = total + p_in[j, owner].astype(jnp.float32)
        p_sum[owner] = total.astype(jnp.bfloat16)
        if k:
            out.send(p_sum.at[owner], x_out.at[fs], x_recv.at[fs], "fs", owner)
        else:
            out.local(p_sum.at[owner], x_out.at[fs])
    for k in order:
        owner = lax.rem(fs + k, n_fs)
        total = g_ref[owner, rep].astype(jnp.float32)
        for j in range(n_rep - 1):
            arrived(g_in.at[j, owner], g_recv.at[j, owner])
            total = total + g_in[j, owner].astype(jnp.float32)
        g_sum[owner] = total.astype(jnp.bfloat16)
        slot = g_out.at[rep, fs]
        if k:
            out.send(g_sum.at[owner], slot, gx_recv.at[rep, fs], "fs", owner)
        else:
            out.local(g_sum.at[owner], slot)
            for j in range(1, n_rep):
                out.send(
                    g_sum.at[owner], slot, gx_recv.at[rep, fs], "rep", lax.rem(rep + j, n_rep)
                )
    for k in near_first(n_fs):
        owner = lax.rem(fs + n_fs - k, n_fs)
        slot = g_out.at[rep, owner]
        arrived(slot, gx_recv.at[rep, owner])
        for j in range(1, n_rep):
            out.send(slot, slot, gx_recv.at[rep, owner], "rep", lax.rem(rep + j, n_rep))
    for k in near_first(n_fs):
        owner = lax.rem(fs + n_fs - k, n_fs)
        arrived(x_out.at[owner], x_recv.at[owner])
    for j in range(1, n_rep):
        half = lax.rem(rep + j, n_rep)
        for k in range(n_fs):
            owner = lax.rem(fs + k, n_fs)
            arrived(g_out.at[half, owner], gx_recv.at[half, owner])
    out.finish()


VMEM = pl.BlockSpec(memory_space=pltpu.VMEM)
ANY = pl.BlockSpec(memory_space=pl.ANY)
DMA = pltpu.SemaphoreType.DMA


def per_device(n_rep, n_fs, n_tp, x, c, gate_weight, up_weight, down_weight):
    bf16, f32 = jnp.bfloat16, jnp.float32
    n_y = max(k for k in range(1, n_fs + 1) if n_fs % k == 0 and k * k <= n_fs)
    n_z = n_fs // n_y
    tokens, width = x.shape
    depth, hidden_tp = gate_weight.shape
    model = width * n_tp
    units = hidden_tp // n_fs
    step = 16 * n_rep
    rows = -(-3 * units // step) * step
    half = rows // n_rep

    w = jnp.concatenate(
        [
            gate_weight.T.reshape(n_fs, units, depth),
            up_weight.T.reshape(n_fs, units, depth),
            down_weight.reshape(n_fs, units, depth),
            jnp.zeros((n_fs, rows - 3 * units, depth), bf16),
        ],
        axis=1,
    ).reshape(n_fs, n_rep, half, depth)
    aligned = depth % 128 == 0
    w_shape = (n_rep, half, model) if aligned else (n_rep, n_fs, half, depth)
    n_sends = (
        2 * ((n_z - 1) + n_z * (n_y - 1) + n_fs * (n_tp - 1) + 1)
        + (n_fs - 1) + n_fs * (n_rep - 1) + 1
    )
    x_all, c_all, w_all = pl.pallas_call(
        functools.partial(gather_kernel, (n_rep, n_fs, n_tp, n_y)),
        out_shape=(
            jax.ShapeDtypeStruct((n_fs, tokens, model), bf16),
            jax.ShapeDtypeStruct((n_fs, tokens, model), bf16),
            jax.ShapeDtypeStruct(w_shape, bf16),
        ),
        in_specs=[VMEM] * 3,
        out_specs=(ANY,) * 3,
        scratch_shapes=[DMA((n_sends,)), DMA((2, n_fs, n_tp)), DMA((n_rep, n_fs))],
        compiler_params=pltpu.CompilerParams(collective_id=0, has_side_effects=True),
    )(x, c, w)
    x_all, c_all = (v.reshape(n_fs * tokens, model) for v in (x_all, c_all))
    if not aligned:
        w_all = w_all.transpose(0, 2, 1, 3)
    w_all = w_all.reshape(rows, model)
    w_in, w_down = w_all[: 2 * units], w_all[2 * units : 3 * units]

    last = (((1,), (1,)), ((), ()))
    first = (((0,), (0,)), ((), ()))
    pre = lax.dot_general(x_all, w_in, last, preferred_element_type=f32)
    grad_hidden = lax.dot_general(c_all, w_down, last, preferred_element_type=f32)
    gate_pre, up_pre = pre[:, :units], pre[:, units:]
    sigmoid_gate = jax.nn.sigmoid(gate_pre)
    activated = gate_pre * sigmoid_gate
    hidden = (activated * up_pre).astype(bf16)
    grad_gate = (
        grad_hidden * up_pre * sigmoid_gate * (1.0 + gate_pre * (1.0 - sigmoid_gate))
    ).astype(bf16)
    grad_up = (grad_hidden * activated).astype(bf16)
    grads = jnp.concatenate([grad_gate, grad_up], axis=1)
    partial = jnp.dot(grads, w_in, preferred_element_type=f32).astype(bf16)
    partial = partial.reshape(n_fs, tokens, model)
    g = jnp.concatenate(
        [
            lax.dot_general(grads, x_all, first, preferred_element_type=f32).astype(bf16),
            lax.dot_general(hidden, c_all, first, preferred_element_type=f32).astype(bf16),
            jnp.zeros((rows - 3 * units, model), bf16),
        ],
        axis=0,
    )
    g = g.reshape(n_rep, half, n_fs, depth).transpose(2, 0, 1, 3)
    n_sends = n_fs * (n_tp - 1) + n_fs * (n_rep - 1) + n_fs + n_fs + n_fs * (n_rep - 1)
    dx, dw = pl.pallas_call(
        functools.partial(scatter_kernel, (n_rep, n_fs, n_tp)),
        out_shape=(
            jax.ShapeDtypeStruct((n_fs, tokens, width), bf16),
            jax.ShapeDtypeStruct((n_rep, n_fs, half, depth), bf16),
        ),
        in_specs=[VMEM] * 2,
        out_specs=(ANY,) * 2,
        scratch_shapes=[
            pltpu.VMEM((n_tp - 1, n_fs, tokens, width), bf16),
            pltpu.VMEM((n_fs, tokens, width), bf16),
            pltpu.VMEM((n_rep - 1, n_fs, half, depth), bf16),
            pltpu.VMEM((n_fs, half, depth), bf16),
            DMA((n_sends,)),
            DMA((n_tp - 1, n_fs)),
            DMA((n_rep - 1, n_fs)),
            DMA((n_fs,)),
            DMA((n_rep, n_fs)),
        ],
        compiler_params=pltpu.CompilerParams(collective_id=1, has_side_effects=True),
    )(partial, g)
    grad_inputs = jnp.sum(dx.astype(f32), axis=0).astype(bf16)
    dw = dw.transpose(1, 0, 2, 3).reshape(n_fs, rows, depth)
    gate_grads, up_grads, down_grads = (
        dw[:, i * units : (i + 1) * units].reshape(hidden_tp, depth) for i in range(3)
    )
    return (
        grad_inputs,
        gate_grads.T.astype(f32),
        up_grads.T.astype(f32),
        down_grads.astype(f32),
    )


def solution(mesh):
    n_rep, n_fs, n_tp = (mesh.shape[axis] for axis in ("rep", "fs", "tp"))
    placed = (
        P(("rep", "fs"), "tp"),
        P(("rep", "fs"), "tp"),
        P("fs", "tp"),
        P("fs", "tp"),
        P("tp", "fs"),
    )
    return jax.shard_map(
        functools.partial(per_device, n_rep, n_fs, n_tp),
        mesh=mesh,
        in_specs=placed,
        out_specs=(P(("rep", "fs"), "tp"), P("fs", "tp"), P("fs", "tp"), P("tp", "fs")),
        check_vma=False,
    )
```

```python
import functools

import jax
import jax.numpy as jnp
from jax import lax
from jax.experimental import pallas as pl
from jax.experimental.pallas import tpu as pltpu
from jax.sharding import PartitionSpec as P

MESH = pl.DeviceIdType.MESH


def enter(n_rep, n_fs, n_tp):
    barrier = pltpu.get_barrier_semaphore()
    for axis, n in (("rep", n_rep), ("fs", n_fs), ("tp", n_tp)):
        me = lax.axis_index(axis)
        for k in range(1, n):
            pl.semaphore_signal(
                barrier, inc=1, device_id={axis: lax.rem(me + k, n)}, device_id_type=MESH
            )
    pl.semaphore_wait(barrier, n_rep + n_fs + n_tp - 3)


class Sender:
    def __init__(self, sems):
        self.sems, self.used, self.pending = sems, 0, []

    def run(self, build, when):
        if when is None:
            build().start()
        else:
            pl.when(when)(lambda: build().start())

    def send(self, src, dst, recv_sem, axis, peer, when=None):
        def build(at=self.used):
            return pltpu.make_async_remote_copy(
                src_ref=src,
                dst_ref=dst,
                send_sem=self.sems.at[at],
                recv_sem=recv_sem,
                device_id={axis: peer},
                device_id_type=MESH,
            )

        self.used += 1
        self.run(build, when)
        self.pending.append((lambda: build().wait_send(), when))

    def local(self, src, dst):
        def build(at=self.used):
            return pltpu.make_async_copy(src, dst, self.sems.at[at])

        self.used += 1
        self.run(build, None)
        self.pending.append((lambda: build().wait(), None))

    def finish(self):
        for wait, when in self.pending:
            if when is None:
                wait()
            else:
                pl.when(when)(wait)


def arrived(slot, recv_sem, when=None):
    def wait():
        pltpu.make_async_copy(slot, slot, recv_sem).wait()

    if when is None:
        wait()
    else:
        pl.when(when)(wait)


def near_first(n):
    return sorted(range(1, n), key=lambda k: min(k, n - k))


def gather_kernel(
    sizes, x_ref, c_ref, w_ref, x_out, c_out, w_out, sends, act_recv, w_recv
):
    n_rep, n_fs, n_tp, n_y = sizes
    n_z = n_fs // n_y
    rep, fs, tp = (lax.axis_index(axis) for axis in ("rep", "fs", "tp"))
    z, y = fs // n_y, lax.rem(fs, n_y)
    width = x_ref.shape[1]
    depth = w_ref.shape[3]
    enter(n_rep, n_fs, n_tp)
    out = Sender(sends)
    acts = ((x_ref, x_out), (c_ref, c_out))

    def act_slot(a, owner, part):
        return acts[a][1].at[owner, :, pl.ds(pl.multiple_of(part * width, width), width)]

    def w_slot(half, owner):
        if depth % 128 == 0:
            return w_out.at[half, :, pl.ds(pl.multiple_of(owner * depth, depth), depth)]
        return w_out.at[half, owner]

    def act_send(a, owner, src, axis, peer, when=None):
        out.send(src, act_slot(a, owner, tp), act_recv.at[a, owner, tp], axis, peer, when)

    def to_tp(a, owner, src, when=None):
        for k in range(1, n_tp):
            act_send(a, owner, src, "tp", lax.rem(tp + k, n_tp), when)

    def to_y(a, owner, src, when=None):
        for k in range(1, n_y):
            act_send(a, owner, src, "fs", z * n_y + lax.rem(y + k, n_y), when)

    for a in range(2):
        src = acts[a][0]
        to_y(a, fs, src)
        act_send(a, fs, src, "fs", fs + n_y, z + 1 < n_z)
        act_send(a, fs, src, "fs", fs - n_y, z >= 1)
    for k in near_first(n_fs):
        peer = lax.rem(fs + k, n_fs)
        out.send(w_ref.at[peer, rep], w_slot(rep, fs), w_recv.at[rep, fs], "fs", peer)
    for k in range(1, n_rep):
        out.send(
            w_ref.at[fs, rep], w_slot(rep, fs), w_recv.at[rep, fs], "rep", lax.rem(rep + k, n_rep)
        )
    for a in range(2):
        to_tp(a, fs, acts[a][0])
        out.local(acts[a][0], act_slot(a, fs, tp))
    out.local(w_ref.at[fs, rep], w_slot(rep, fs))

    def swap_weights():
        for k in near_first(n_fs):
            owner = lax.rem(fs + n_fs - k, n_fs)
            slot = w_slot(rep, owner)
            arrived(slot, w_recv.at[rep, owner])
            for j in range(1, n_rep):
                peer = lax.rem(rep + j, n_rep)
                out.send(slot, slot, w_recv.at[rep, owner], "rep", peer)

    for k in range(1, n_z):
        if k == max(n_z - 1, 1):
            swap_weights()
        for a in range(2):
            for here, onward, step in (
                (z >= k, z + 1 < n_z, -1), (z + k < n_z, z >= 1, 1)
            ):
                owner = fs + step * k * n_y
                slot = act_slot(a, owner, tp)
                arrived(slot, act_recv.at[a, owner, tp], here)
                if k < n_z - 1:
                    act_send(
                        a, owner, slot, "fs", fs - step * n_y, jnp.logical_and(here, onward)
                    )
                to_y(a, owner, slot, here)
                to_tp(a, owner, slot, here)
    if n_z == 1:
        swap_weights()
    for kz in [0] + near_first(n_z):
        for ky in range(1, n_y):
            owner = lax.rem(z + n_z - kz, n_z) * n_y + lax.rem(y + ky, n_y)
            for a in range(2):
                slot = act_slot(a, owner, tp)
                arrived(slot, act_recv.at[a, owner, tp])
                to_tp(a, owner, slot)
    for j in range(1, n_rep):
        half = lax.rem(rep + j, n_rep)
        for k in range(n_fs):
            owner = lax.rem(fs + k, n_fs)
            arrived(w_slot(half, owner), w_recv.at[half, owner])
    for j in range(1, n_tp):
        part = lax.rem(tp + j, n_tp)
        for k in range(n_fs):
            owner = lax.rem(fs + k, n_fs)
            for a in range(2):
                arrived(act_slot(a, owner, part), act_recv.at[a, owner, part])
    out.finish()


def scatter_kernel(
    sizes, d_ref, w_ref, g_ref, x_ref, g_out,
    p, p_in, q, y_in, r, x_in, g_in, g_sum, sends, p_recv, y_recv, x_recv, g_recv, gx_recv,
):
    n_rep, n_fs, n_tp, n_y = sizes
    n_z = n_fs // n_y
    f32, bf16 = jnp.float32, jnp.bfloat16
    rep, fs, tp = (lax.axis_index(axis) for axis in ("rep", "fs", "tp"))
    z, y = fs // n_y, lax.rem(fs, n_y)
    rows, width = x_ref.shape
    depth = g_sum.shape[2]
    enter(n_rep, n_fs, n_tp)
    out = Sender(sends)
    order = near_first(n_fs) + [0]
    zs = near_first(n_z) + [0]

    def columns(part, size):
        return pl.ds(pl.multiple_of(part * size, size), size)

    def g_part(owner, half):
        if depth % 128 == 0:
            return g_ref.at[half, :, columns(owner, depth)]
        return g_ref.at[half, owner]

    for k in order:
        owner = lax.rem(fs + k, n_fs)
        for j in range(1, n_rep):
            peer = lax.rem(rep + j, n_rep)
            out.send(
                g_part(owner, peer), g_in.at[j - 1, owner], g_recv.at[j - 1, owner], "rep", peer
            )
    blocks = [(kz, ky) for ky in list(range(1, n_y)) + [0] for kz in zs]

    def owner_of(kz, ky):
        return lax.rem(z + kz, n_z) * n_y + lax.rem(y + ky, n_y)

    for block in blocks:
        owner = owner_of(*block)
        p[owner] = jnp.dot(d_ref[owner], w_ref[...], preferred_element_type=f32).astype(bf16)
        for j in range(1, n_tp):
            peer = lax.rem(tp + j, n_tp)
            out.send(
                p.at[owner, :, columns(peer, width)],
                p_in.at[j - 1, owner],
                p_recv.at[j - 1, owner],
                "tp",
                peer,
            )

    def pair_sum(owner):
        total = p[owner, :, columns(tp, width)].astype(f32)
        for j in range(n_tp - 1):
            arrived(p_in.at[j, owner], p_recv.at[j, owner])
            total = total + p_in[j, owner].astype(f32)
        return total

    def g_step(k):
        owner = lax.rem(fs + k, n_fs)
        total = g_part(owner, rep)[...].astype(f32)
        for j in range(n_rep - 1):
            arrived(g_in.at[j, owner], g_recv.at[j, owner])
            total = total + g_in[j, owner].astype(f32)
        g_sum[owner] = total.astype(bf16)
        slot = g_out.at[rep, fs]
        if k:
            out.send(g_sum.at[owner], slot, gx_recv.at[rep, fs], "fs", owner)
        else:
            out.local(g_sum.at[owner], slot)
            for j in range(1, n_rep):
                out.send(
                    g_sum.at[owner], slot, gx_recv.at[rep, fs], "rep", lax.rem(rep + j, n_rep)
                )

    for kz, ky in blocks:
        if ky:
            owner = owner_of(kz, ky)
            q[owner] = pair_sum(owner).astype(bf16)
            at = (ky - 1, lax.rem(z + kz, n_z))
            out.send(
                q.at[owner], y_in.at[at], y_recv.at[at], "fs", z * n_y + lax.rem(y + ky, n_y)
            )
    early = len(order) // 2
    for k in order[:early]:
        g_step(k)
    for kz in zs:
        owner = owner_of(kz, 0)
        z_to = lax.rem(z + kz, n_z)
        total = pair_sum(owner)
        for ky in range(1, n_y):
            at = (ky - 1, z_to)
            arrived(y_in.at[at], y_recv.at[at])
            total = total + y_in[at].astype(f32)
        if kz:
            r[z_to] = total.astype(bf16)
            out.send(r.at[z_to], x_in.at[z], x_recv.at[z], "fs", owner)
        else:
            own = total
            x_in[z] = own.astype(bf16)
    for k in order[early:]:
        g_step(k)
    for k in near_first(n_fs):
        owner = lax.rem(fs + n_fs - k, n_fs)
        slot = g_out.at[rep, owner]
        arrived(slot, gx_recv.at[rep, owner])
        for j in range(1, n_rep):
            out.send(slot, slot, gx_recv.at[rep, owner], "rep", lax.rem(rep + j, n_rep))
    for kz in near_first(n_z):
        z_from = lax.rem(z + n_z - kz, n_z)
        arrived(x_in.at[z_from], x_recv.at[z_from])
    total = x_in[0].astype(f32)
    for k in range(1, n_z):
        total = total + x_in[k].astype(f32)
    x_ref[...] = total.astype(bf16)
    for j in range(1, n_rep):
        half = lax.rem(rep + j, n_rep)
        for k in range(n_fs):
            owner = lax.rem(fs + k, n_fs)
            arrived(g_out.at[half, owner], gx_recv.at[half, owner])
    out.finish()


VMEM = pl.BlockSpec(memory_space=pltpu.VMEM)
ANY = pl.BlockSpec(memory_space=pl.ANY)
DMA = pltpu.SemaphoreType.DMA


def per_device(n_rep, n_fs, n_tp, x, c, gate_weight, up_weight, down_weight):
    bf16, f32 = jnp.bfloat16, jnp.float32
    n_y = max(k for k in range(1, n_fs + 1) if n_fs % k == 0 and k * k <= n_fs)
    n_z = n_fs // n_y
    tokens, width = x.shape
    depth, hidden_tp = gate_weight.shape
    model = width * n_tp
    units = hidden_tp // n_fs
    step = 16 * n_rep
    rows = -(-3 * units // step) * step
    half = rows // n_rep

    w = jnp.concatenate(
        [
            gate_weight.T.reshape(n_fs, units, depth),
            up_weight.T.reshape(n_fs, units, depth),
            down_weight.reshape(n_fs, units, depth),
            jnp.zeros((n_fs, rows - 3 * units, depth), bf16),
        ],
        axis=1,
    ).reshape(n_fs, n_rep, half, depth)
    aligned = depth % 128 == 0
    w_shape = (n_rep, half, model) if aligned else (n_rep, n_fs, half, depth)
    n_sends = (
        2 * (2 + (2 * n_z - 1) * (n_y - 1) + (2 * n_z - 1) * (n_tp - 1) + 2 * n_z + n_fs * (n_tp - 1) + 1)
        + (n_fs - 1) + n_fs * (n_rep - 1) + 1
    )
    x_all, c_all, w_all = pl.pallas_call(
        functools.partial(gather_kernel, (n_rep, n_fs, n_tp, n_y)),
        out_shape=(
            jax.ShapeDtypeStruct((n_fs, tokens, model), bf16),
            jax.ShapeDtypeStruct((n_fs, tokens, model), bf16),
            jax.ShapeDtypeStruct(w_shape, bf16),
        ),
        in_specs=[VMEM] * 3,
        out_specs=(ANY,) * 3,
        scratch_shapes=[DMA((n_sends,)), DMA((2, n_fs, n_tp)), DMA((n_rep, n_fs))],
        compiler_params=pltpu.CompilerParams(collective_id=0, has_side_effects=True),
    )(x, c, w)
    x_all, c_all = (v.reshape(n_fs * tokens, model) for v in (x_all, c_all))
    if not aligned:
        w_all = w_all.transpose(0, 2, 1, 3)
    w_all = w_all.reshape(rows, model)
    w_in, w_down = w_all[: 2 * units], w_all[2 * units : 3 * units]

    last = (((1,), (1,)), ((), ()))
    first = (((0,), (0,)), ((), ()))
    pre = lax.dot_general(x_all, w_in, last, preferred_element_type=f32)
    grad_hidden = lax.dot_general(c_all, w_down, last, preferred_element_type=f32)
    gate_pre, up_pre = pre[:, :units], pre[:, units:]
    sigmoid_gate = jax.nn.sigmoid(gate_pre)
    activated = gate_pre * sigmoid_gate
    hidden = (activated * up_pre).astype(bf16)
    grad_gate = (
        grad_hidden * up_pre * sigmoid_gate * (1.0 + gate_pre * (1.0 - sigmoid_gate))
    ).astype(bf16)
    grad_up = (grad_hidden * activated).astype(bf16)
    grads = jnp.concatenate([grad_gate, grad_up], axis=1)
    g = jnp.concatenate(
        [
            lax.dot_general(grads, x_all, first, preferred_element_type=f32).astype(bf16),
            lax.dot_general(hidden, c_all, first, preferred_element_type=f32).astype(bf16),
            jnp.zeros((rows - 3 * units, model), bf16),
        ],
        axis=0,
    )
    g = g.reshape(w_shape if aligned else (n_rep, half, n_fs, depth))
    if not aligned:
        g = g.transpose(0, 2, 1, 3)
    n_sends = n_fs * (n_tp - 1) + 2 * n_fs * (n_rep - 1) + 3 * n_fs
    grad_inputs, dw = pl.pallas_call(
        functools.partial(scatter_kernel, (n_rep, n_fs, n_tp, n_y)),
        out_shape=(
            jax.ShapeDtypeStruct((tokens, width), bf16),
            jax.ShapeDtypeStruct((n_rep, n_fs, half, depth), bf16),
        ),
        in_specs=[VMEM] * 3,
        out_specs=(VMEM, ANY),
        scratch_shapes=[
            pltpu.VMEM((n_fs, tokens, model), bf16),
            pltpu.VMEM((n_tp - 1, n_fs, tokens, width), bf16),
            pltpu.VMEM((n_fs, tokens, width), bf16),
            pltpu.VMEM((n_y - 1, n_z, tokens, width), bf16),
            pltpu.VMEM((n_z, tokens, width), bf16),
            pltpu.VMEM((n_z, tokens, width), bf16),
            pltpu.VMEM((n_rep - 1, n_fs, half, depth), bf16),
            pltpu.VMEM((n_fs, half, depth), bf16),
            DMA((n_sends,)),
            DMA((n_tp - 1, n_fs)),
            DMA((n_y - 1, n_z)),
            DMA((n_z,)),
            DMA((n_rep - 1, n_fs)),
            DMA((n_rep, n_fs)),
        ],
        compiler_params=pltpu.CompilerParams(
            collective_id=1, has_side_effects=True, vmem_limit_bytes=60 * 2**20
        ),
    )(grads.reshape(n_fs, tokens, 2 * units), w_in, g)
    dw = dw.transpose(1, 0, 2, 3).reshape(n_fs, rows, depth)
    gate_grads, up_grads, down_grads = (
        dw[:, i * units : (i + 1) * units].reshape(hidden_tp, depth) for i in range(3)
    )
    return (
        grad_inputs,
        gate_grads.T.astype(f32),
        up_grads.T.astype(f32),
        down_grads.astype(f32),
    )


def solution(mesh):
    n_rep, n_fs, n_tp = (mesh.shape[axis] for axis in ("rep", "fs", "tp"))
    placed = (
        P(("rep", "fs"), "tp"),
        P(("rep", "fs"), "tp"),
        P("fs", "tp"),
        P("fs", "tp"),
        P("tp", "fs"),
    )
    return jax.shard_map(
        functools.partial(per_device, n_rep, n_fs, n_tp),
        mesh=mesh,
        in_specs=placed,
        out_specs=(P(("rep", "fs"), "tp"), P("fs", "tp"), P("fs", "tp"), P("tp", "fs")),
        check_vma=False,
    )
```

```python
import functools

import jax
import jax.numpy as jnp
from jax import lax
from jax.experimental import pallas as pl
from jax.experimental.pallas import tpu as pltpu
from jax.sharding import PartitionSpec as P

MESH = pl.DeviceIdType.MESH


def enter(n_rep, n_fs, n_tp):
    barrier = pltpu.get_barrier_semaphore()
    for axis, n in (("rep", n_rep), ("fs", n_fs), ("tp", n_tp)):
        me = lax.axis_index(axis)
        for k in range(1, n):
            pl.semaphore_signal(
                barrier, inc=1, device_id={axis: lax.rem(me + k, n)}, device_id_type=MESH
            )
    pl.semaphore_wait(barrier, n_rep + n_fs + n_tp - 3)


class Sender:
    def __init__(self, sems):
        self.sems, self.used, self.pending = sems, 0, []

    def run(self, build, when):
        if when is None:
            build().start()
        else:
            pl.when(when)(lambda: build().start())

    def send(self, src, dst, recv_sem, axis, peer, when=None):
        def build(at=self.used):
            return pltpu.make_async_remote_copy(
                src_ref=src,
                dst_ref=dst,
                send_sem=self.sems.at[at],
                recv_sem=recv_sem,
                device_id={axis: peer},
                device_id_type=MESH,
            )

        self.used += 1
        self.run(build, when)
        self.pending.append((lambda: build().wait_send(), when))

    def local(self, src, dst):
        def build(at=self.used):
            return pltpu.make_async_copy(src, dst, self.sems.at[at])

        self.used += 1
        self.run(build, None)
        self.pending.append((lambda: build().wait(), None))

    def finish(self):
        for wait, when in self.pending:
            if when is None:
                wait()
            else:
                pl.when(when)(wait)


def arrived(slot, recv_sem, when=None):
    def wait():
        pltpu.make_async_copy(slot, slot, recv_sem).wait()

    if when is None:
        wait()
    else:
        pl.when(when)(wait)


def near_first(n):
    return sorted(range(1, n), key=lambda k: min(k, n - k))


def split_weights(weights, w_ref):
    n_fs, n_rep, half, depth = w_ref.shape
    units = weights[2].shape[0] // n_fs
    turned = [weights[0][...].T, weights[1][...].T, weights[2][...]]
    for owner in range(n_fs):
        for i, value in enumerate(turned):
            for h in range(n_rep):
                low, high = max(i * units, h * half), min((i + 1) * units, (h + 1) * half)
                if low < high:
                    start = owner * units - i * units
                    w_ref[owner, h, low - h * half : high - h * half] = value[
                        start + low : start + high
                    ]
        used = 3 * units - (n_rep - 1) * half
        w_ref[owner, n_rep - 1, used:] = jnp.zeros((half - used, depth), w_ref.dtype)


def gather_kernel(
    sizes, x_ref, c_ref, *refs
):
    *weights, x_out, c_out, w_out, w_ref, sends, act_recv, w_recv = refs
    n_rep, n_fs, n_tp, n_y = sizes
    n_z = n_fs // n_y
    rep, fs, tp = (lax.axis_index(axis) for axis in ("rep", "fs", "tp"))
    z, y = fs // n_y, lax.rem(fs, n_y)
    width = x_ref.shape[1]
    depth = w_ref.shape[3]
    enter(n_rep, n_fs, n_tp)
    out = Sender(sends)
    acts = ((x_ref, x_out), (c_ref, c_out))

    def act_slot(a, owner, part):
        return acts[a][1].at[owner, :, pl.ds(pl.multiple_of(part * width, width), width)]

    def w_slot(half, owner):
        if depth % 128 == 0:
            return w_out.at[half, :, pl.ds(pl.multiple_of(owner * depth, depth), depth)]
        return w_out.at[half, owner]

    def act_send(a, owner, src, axis, peer, when=None):
        out.send(src, act_slot(a, owner, tp), act_recv.at[a, owner, tp], axis, peer, when)

    def to_tp(a, owner, src, when=None):
        for k in range(1, n_tp):
            act_send(a, owner, src, "tp", lax.rem(tp + k, n_tp), when)

    def to_y(a, owner, src, when=None):
        for k in range(1, n_y):
            act_send(a, owner, src, "fs", z * n_y + lax.rem(y + k, n_y), when)

    for a in range(2):
        src = acts[a][0]
        to_y(a, fs, src)
        act_send(a, fs, src, "fs", fs + n_y, z + 1 < n_z)
        act_send(a, fs, src, "fs", fs - n_y, z >= 1)
    for a in range(2):
        to_tp(a, fs, acts[a][0])
        out.local(acts[a][0], act_slot(a, fs, tp))
    if len(weights) == 1:
        w_ref = weights[0]
    else:
        split_weights(weights, w_ref)
    for k in near_first(n_fs):
        peer = lax.rem(fs + k, n_fs)
        out.send(w_ref.at[peer, rep], w_slot(rep, fs), w_recv.at[rep, fs], "fs", peer)
    for k in range(1, n_rep):
        out.send(
            w_ref.at[fs, rep], w_slot(rep, fs), w_recv.at[rep, fs], "rep", lax.rem(rep + k, n_rep)
        )
    out.local(w_ref.at[fs, rep], w_slot(rep, fs))

    def swap_weights():
        for k in near_first(n_fs):
            owner = lax.rem(fs + n_fs - k, n_fs)
            slot = w_slot(rep, owner)
            arrived(slot, w_recv.at[rep, owner])
            for j in range(1, n_rep):
                peer = lax.rem(rep + j, n_rep)
                out.send(slot, slot, w_recv.at[rep, owner], "rep", peer)

    for k in range(1, n_z):
        if k == max(n_z - 1, 1):
            swap_weights()
        for a in range(2):
            for here, onward, step in (
                (z >= k, z + 1 < n_z, -1), (z + k < n_z, z >= 1, 1)
            ):
                owner = fs + step * k * n_y
                slot = act_slot(a, owner, tp)
                arrived(slot, act_recv.at[a, owner, tp], here)
                if k < n_z - 1:
                    act_send(
                        a, owner, slot, "fs", fs - step * n_y, jnp.logical_and(here, onward)
                    )
                to_y(a, owner, slot, here)
                to_tp(a, owner, slot, here)
    if n_z == 1:
        swap_weights()
    for kz in [0] + near_first(n_z):
        for ky in range(1, n_y):
            owner = lax.rem(z + n_z - kz, n_z) * n_y + lax.rem(y + ky, n_y)
            for a in range(2):
                slot = act_slot(a, owner, tp)
                arrived(slot, act_recv.at[a, owner, tp])
                to_tp(a, owner, slot)
    for j in range(1, n_rep):
        half = lax.rem(rep + j, n_rep)
        for k in range(n_fs):
            owner = lax.rem(fs + k, n_fs)
            arrived(w_slot(half, owner), w_recv.at[half, owner])
    for j in range(1, n_tp):
        part = lax.rem(tp + j, n_tp)
        for k in range(n_fs):
            owner = lax.rem(fs + k, n_fs)
            for a in range(2):
                arrived(act_slot(a, owner, part), act_recv.at[a, owner, part])
    out.finish()


def scatter_kernel(
    sizes, d_ref, w_ref, g_ref, x_ref, g_out,
    p, p_in, q, y_in, r, x_in, g_in, g_sum, sends, p_recv, y_recv, x_recv, g_recv, gx_recv,
):
    n_rep, n_fs, n_tp, n_y = sizes
    n_z = n_fs // n_y
    f32, bf16 = jnp.float32, jnp.bfloat16
    rep, fs, tp = (lax.axis_index(axis) for axis in ("rep", "fs", "tp"))
    z, y = fs // n_y, lax.rem(fs, n_y)
    rows, width = x_ref.shape
    depth = g_sum.shape[2]
    enter(n_rep, n_fs, n_tp)
    out = Sender(sends)
    order = near_first(n_fs) + [0]
    zs = near_first(n_z) + [0]

    def columns(part, size):
        return pl.ds(pl.multiple_of(part * size, size), size)

    def g_part(owner, half):
        if depth % 128 == 0:
            return g_ref.at[half, :, columns(owner, depth)]
        return g_ref.at[half, owner]

    for k in order:
        owner = lax.rem(fs + k, n_fs)
        for j in range(1, n_rep):
            peer = lax.rem(rep + j, n_rep)
            out.send(
                g_part(owner, peer), g_in.at[j - 1, owner], g_recv.at[j - 1, owner], "rep", peer
            )
    blocks = [(kz, ky) for ky in list(range(1, n_y)) + [0] for kz in zs]

    def owner_of(kz, ky):
        return lax.rem(z + kz, n_z) * n_y + lax.rem(y + ky, n_y)

    for block in blocks:
        owner = owner_of(*block)
        p[owner] = jnp.dot(
            d_ref[owner], w_ref[: d_ref.shape[2]], preferred_element_type=f32
        ).astype(bf16)
        for j in range(1, n_tp):
            peer = lax.rem(tp + j, n_tp)
            out.send(
                p.at[owner, :, columns(peer, width)],
                p_in.at[j - 1, owner],
                p_recv.at[j - 1, owner],
                "tp",
                peer,
            )

    def pair_sum(owner):
        total = p[owner, :, columns(tp, width)].astype(f32)
        for j in range(n_tp - 1):
            arrived(p_in.at[j, owner], p_recv.at[j, owner])
            total = total + p_in[j, owner].astype(f32)
        return total

    def g_step(k):
        owner = lax.rem(fs + k, n_fs)
        total = g_part(owner, rep)[...].astype(f32)
        for j in range(n_rep - 1):
            arrived(g_in.at[j, owner], g_recv.at[j, owner])
            total = total + g_in[j, owner].astype(f32)
        g_sum[owner] = total.astype(bf16)
        slot = g_out.at[fs, rep]
        if k:
            out.send(g_sum.at[owner], slot, gx_recv.at[rep, fs], "fs", owner)
        else:
            out.local(g_sum.at[owner], slot)
            for j in range(1, n_rep):
                out.send(
                    g_sum.at[owner], slot, gx_recv.at[rep, fs], "rep", lax.rem(rep + j, n_rep)
                )

    for kz, ky in blocks:
        if ky:
            owner = owner_of(kz, ky)
            q[owner] = pair_sum(owner).astype(bf16)
            at = (ky - 1, lax.rem(z + kz, n_z))
            out.send(
                q.at[owner], y_in.at[at], y_recv.at[at], "fs", z * n_y + lax.rem(y + ky, n_y)
            )
    def x_step(kz):
        owner = owner_of(kz, 0)
        z_to = lax.rem(z + kz, n_z)
        total = pair_sum(owner)
        for ky in range(1, n_y):
            at = (ky - 1, z_to)
            arrived(y_in.at[at], y_recv.at[at])
            total = total + y_in[at].astype(f32)
        if kz:
            r[z_to] = total.astype(bf16)
            out.send(r.at[z_to], x_in.at[z], x_recv.at[z], "fs", owner)
        else:
            x_in[z] = total.astype(bf16)

    def g_forward(k):
        if k:
            owner = lax.rem(fs + n_fs - k, n_fs)
            slot = g_out.at[owner, rep]
            arrived(slot, gx_recv.at[rep, owner])
            for j in range(1, n_rep):
                out.send(slot, slot, gx_recv.at[rep, owner], "rep", lax.rem(rep + j, n_rep))

    for i, kz in enumerate(zs):
        for k in order[i * n_y : (i + 1) * n_y]:
            g_step(k)
        x_step(kz)
        if i:
            for k in order[(i - 1) * n_y : i * n_y]:
                g_forward(k)
    for k in order[-n_y:]:
        g_forward(k)
    for kz in near_first(n_z):
        z_from = lax.rem(z + n_z - kz, n_z)
        arrived(x_in.at[z_from], x_recv.at[z_from])
    total = x_in[0].astype(f32)
    for k in range(1, n_z):
        total = total + x_in[k].astype(f32)
    x_ref[...] = total.astype(bf16)
    for j in range(1, n_rep):
        half = lax.rem(rep + j, n_rep)
        for k in range(n_fs):
            owner = lax.rem(fs + k, n_fs)
            arrived(g_out.at[owner, half], gx_recv.at[half, owner])
    out.finish()


VMEM = pl.BlockSpec(memory_space=pltpu.VMEM)
ANY = pl.BlockSpec(memory_space=pl.ANY)
DMA = pltpu.SemaphoreType.DMA


def per_device(n_rep, n_fs, n_tp, x, c, gate_weight, up_weight, down_weight):
    bf16, f32 = jnp.bfloat16, jnp.float32
    n_y = max(k for k in range(1, n_fs + 1) if n_fs % k == 0 and k * k <= n_fs)
    n_z = n_fs // n_y
    tokens, width = x.shape
    depth, hidden_tp = gate_weight.shape
    model = width * n_tp
    units = hidden_tp // n_fs
    step = 16 * n_rep
    rows = -(-3 * units // step) * step
    half = rows // n_rep

    weights = [gate_weight, up_weight, down_weight]
    if units % 16 or depth % 128 or 3 * units <= rows - half:
        blocks = [gate_weight.T, up_weight.T, down_weight]
        blocks = [v.reshape(n_fs, units, depth) for v in blocks]
        blocks.append(jnp.zeros((n_fs, rows - 3 * units, depth), bf16))
        weights = [jnp.concatenate(blocks, axis=1).reshape(n_fs, n_rep, half, depth)]
    aligned = depth % 128 == 0
    w_shape = (n_rep, half, model) if aligned else (n_rep, n_fs, half, depth)
    n_sends = (
        2 * (2 + (2 * n_z - 1) * (n_y - 1) + (2 * n_z - 1) * (n_tp - 1) + 2 * n_z + n_fs * (n_tp - 1) + 1)
        + (n_fs - 1) + n_fs * (n_rep - 1) + 1
    )
    x_all, c_all, w_all = pl.pallas_call(
        functools.partial(gather_kernel, (n_rep, n_fs, n_tp, n_y)),
        out_shape=(
            jax.ShapeDtypeStruct((n_fs, tokens, model), bf16),
            jax.ShapeDtypeStruct((n_fs, tokens, model), bf16),
            jax.ShapeDtypeStruct(w_shape, bf16),
        ),
        in_specs=[VMEM] * (2 + len(weights)),
        out_specs=(ANY,) * 3,
        scratch_shapes=[pltpu.VMEM((n_fs, n_rep, half, depth), bf16), DMA((n_sends,)), DMA((2, n_fs, n_tp)), DMA((n_rep, n_fs))],
        compiler_params=pltpu.CompilerParams(collective_id=0, has_side_effects=True),
    )(x, c, *weights)
    x_all, c_all = (v.reshape(n_fs * tokens, model) for v in (x_all, c_all))
    if not aligned:
        w_all = w_all.transpose(0, 2, 1, 3)
    w_all = w_all.reshape(rows, model)
    w_in, w_down = w_all[: 2 * units], w_all[2 * units : 3 * units]

    last = (((1,), (1,)), ((), ()))
    first = (((0,), (0,)), ((), ()))
    pre = lax.dot_general(x_all, w_in, last, preferred_element_type=f32)
    grad_hidden = lax.dot_general(c_all, w_down, last, preferred_element_type=f32)
    gate_pre, up_pre = pre[:, :units], pre[:, units:]
    sigmoid_gate = jax.nn.sigmoid(gate_pre)
    activated = gate_pre * sigmoid_gate
    hidden = (activated * up_pre).astype(bf16)
    grad_gate = (
        grad_hidden * up_pre * sigmoid_gate * (1.0 + gate_pre * (1.0 - sigmoid_gate))
    ).astype(bf16)
    grad_up = (grad_hidden * activated).astype(bf16)
    grads = jnp.concatenate([grad_gate, grad_up], axis=1)
    g = jnp.concatenate(
        [
            lax.dot_general(grads, x_all, first, preferred_element_type=f32).astype(bf16),
            lax.dot_general(hidden, c_all, first, preferred_element_type=f32).astype(bf16),
            jnp.zeros((rows - 3 * units, model), bf16),
        ],
        axis=0,
    )
    g = g.reshape(w_shape if aligned else (n_rep, half, n_fs, depth))
    if not aligned:
        g = g.transpose(0, 2, 1, 3)
    n_sends = n_fs * (n_tp - 1) + 2 * n_fs * (n_rep - 1) + 3 * n_fs
    grad_inputs, dw = pl.pallas_call(
        functools.partial(scatter_kernel, (n_rep, n_fs, n_tp, n_y)),
        out_shape=(
            jax.ShapeDtypeStruct((tokens, width), bf16),
            jax.ShapeDtypeStruct((n_fs, n_rep, half, depth), bf16),
        ),
        in_specs=[VMEM] * 3,
        out_specs=(VMEM, ANY),
        scratch_shapes=[
            pltpu.VMEM((n_fs, tokens, model), bf16),
            pltpu.VMEM((n_tp - 1, n_fs, tokens, width), bf16),
            pltpu.VMEM((n_fs, tokens, width), bf16),
            pltpu.VMEM((n_y - 1, n_z, tokens, width), bf16),
            pltpu.VMEM((n_z, tokens, width), bf16),
            pltpu.VMEM((n_z, tokens, width), bf16),
            pltpu.VMEM((n_rep - 1, n_fs, half, depth), bf16),
            pltpu.VMEM((n_fs, half, depth), bf16),
            DMA((n_sends,)),
            DMA((n_tp - 1, n_fs)),
            DMA((n_y - 1, n_z)),
            DMA((n_z,)),
            DMA((n_rep - 1, n_fs)),
            DMA((n_rep, n_fs)),
        ],
        compiler_params=pltpu.CompilerParams(
            collective_id=1, has_side_effects=True, vmem_limit_bytes=60 * 2**20
        ),
    )(grads.reshape(n_fs, tokens, 2 * units), w_all, g)
    dw = dw.reshape(n_fs, rows, depth)
    gate_grads, up_grads, down_grads = (
        dw[:, i * units : (i + 1) * units].reshape(hidden_tp, depth) for i in range(3)
    )
    return (
        grad_inputs,
        gate_grads.T.astype(f32),
        up_grads.T.astype(f32),
        down_grads.astype(f32),
    )


def solution(mesh):
    n_rep, n_fs, n_tp = (mesh.shape[axis] for axis in ("rep", "fs", "tp"))
    placed = (
        P(("rep", "fs"), "tp"),
        P(("rep", "fs"), "tp"),
        P("fs", "tp"),
        P("fs", "tp"),
        P("tp", "fs"),
    )
    return jax.shard_map(
        functools.partial(per_device, n_rep, n_fs, n_tp),
        mesh=mesh,
        in_specs=placed,
        out_specs=(P(("rep", "fs"), "tp"), P("fs", "tp"), P("fs", "tp"), P("tp", "fs")),
        check_vma=False,
    )
```

```python
import functools

import jax
import jax.numpy as jnp
from jax import lax
from jax.experimental import pallas as pl
from jax.experimental.pallas import tpu as pltpu
from jax.sharding import PartitionSpec as P

MESH = pl.DeviceIdType.MESH


def enter(n_rep, n_fs, n_tp):
    barrier = pltpu.get_barrier_semaphore()
    for axis, n in (("rep", n_rep), ("fs", n_fs), ("tp", n_tp)):
        me = lax.axis_index(axis)
        for k in range(1, n):
            pl.semaphore_signal(
                barrier, inc=1, device_id={axis: lax.rem(me + k, n)}, device_id_type=MESH
            )
    pl.semaphore_wait(barrier, n_rep + n_fs + n_tp - 3)


class Sender:
    def __init__(self, sems):
        self.sems, self.used, self.pending = sems, 0, []

    def run(self, build, when):
        if when is None:
            build().start()
        else:
            pl.when(when)(lambda: build().start())

    def send(self, src, dst, recv_sem, axis, peer, when=None):
        def build(at=self.used):
            return pltpu.make_async_remote_copy(
                src_ref=src,
                dst_ref=dst,
                send_sem=self.sems.at[at],
                recv_sem=recv_sem,
                device_id={axis: peer},
                device_id_type=MESH,
            )

        self.used += 1
        self.run(build, when)
        self.pending.append((lambda: build().wait_send(), when))

    def local(self, src, dst):
        def build(at=self.used):
            return pltpu.make_async_copy(src, dst, self.sems.at[at])

        self.used += 1
        self.run(build, None)
        self.pending.append((lambda: build().wait(), None))

    def finish(self):
        for wait, when in self.pending:
            if when is None:
                wait()
            else:
                pl.when(when)(wait)


def arrived(slot, recv_sem, when=None):
    def wait():
        pltpu.make_async_copy(slot, slot, recv_sem).wait()

    if when is None:
        wait()
    else:
        pl.when(when)(wait)


def near_first(n):
    return sorted(range(1, n), key=lambda k: min(k, n - k))


def split_weights(weights, w_ref):
    n_fs, n_rep, half, depth = w_ref.shape
    units = weights[2].shape[0] // n_fs
    turned = [weights[0][...].T, weights[1][...].T, weights[2][...]]
    for owner in range(n_fs):
        for i, value in enumerate(turned):
            for h in range(n_rep):
                low, high = max(i * units, h * half), min((i + 1) * units, (h + 1) * half)
                if low < high:
                    start = owner * units - i * units
                    w_ref[owner, h, low - h * half : high - h * half] = value[
                        start + low : start + high
                    ]
        used = 3 * units - (n_rep - 1) * half
        w_ref[owner, n_rep - 1, used:] = jnp.zeros((half - used, depth), w_ref.dtype)


def gather_kernel(
    sizes, x_ref, c_ref, *refs
):
    *weights, x_out, c_out, w_out, w_ref, sends, act_recv, w_recv = refs
    n_rep, n_fs, n_tp, n_y = sizes
    n_z = n_fs // n_y
    rep, fs, tp = (lax.axis_index(axis) for axis in ("rep", "fs", "tp"))
    z, y = fs // n_y, lax.rem(fs, n_y)
    width = x_ref.shape[1]
    depth = w_ref.shape[3]
    enter(n_rep, n_fs, n_tp)
    out = Sender(sends)
    acts = ((x_ref, x_out), (c_ref, c_out))

    def act_slot(a, owner, part):
        return acts[a][1].at[owner, :, pl.ds(pl.multiple_of(part * width, width), width)]

    def w_slot(half, owner):
        if depth % 128 == 0:
            return w_out.at[half, :, pl.ds(pl.multiple_of(owner * depth, depth), depth)]
        return w_out.at[half, owner]

    def act_send(a, owner, src, axis, peer, when=None):
        out.send(src, act_slot(a, owner, tp), act_recv.at[a, owner, tp], axis, peer, when)

    def to_tp(a, owner, src, when=None):
        for k in range(1, n_tp):
            act_send(a, owner, src, "tp", lax.rem(tp + k, n_tp), when)

    def to_y(a, owner, src, when=None):
        for k in range(1, n_y):
            act_send(a, owner, src, "fs", z * n_y + lax.rem(y + k, n_y), when)

    for a in range(2):
        src = acts[a][0]
        to_y(a, fs, src)
        act_send(a, fs, src, "fs", fs + n_y, z + 1 < n_z)
        act_send(a, fs, src, "fs", fs - n_y, z >= 1)
    for a in range(2):
        to_tp(a, fs, acts[a][0])
        out.local(acts[a][0], act_slot(a, fs, tp))
    if len(weights) == 1:
        w_ref = weights[0]
    else:
        split_weights(weights, w_ref)
    offsets = near_first(n_fs)
    soon, late = offsets[: len(offsets) // 2], offsets[len(offsets) // 2 :]
    if n_z < 3:
        soon, late = [], offsets

    def send_weights(group):
        for k in group:
            peer = lax.rem(fs + k, n_fs)
            out.send(w_ref.at[peer, rep], w_slot(rep, fs), w_recv.at[rep, fs], "fs", peer)

    if n_z < 3:
        send_weights(late)
    for k in range(1, n_rep):
        out.send(
            w_ref.at[fs, rep], w_slot(rep, fs), w_recv.at[rep, fs], "rep", lax.rem(rep + k, n_rep)
        )
    out.local(w_ref.at[fs, rep], w_slot(rep, fs))

    def swap_weights(group):
        for k in group:
            owner = lax.rem(fs + n_fs - k, n_fs)
            slot = w_slot(rep, owner)
            arrived(slot, w_recv.at[rep, owner])
            for j in range(1, n_rep):
                peer = lax.rem(rep + j, n_rep)
                out.send(slot, slot, w_recv.at[rep, owner], "rep", peer)

    for k in range(1, n_z):
        if k == n_z - 1:
            swap_weights(soon)
        for a in range(2):
            for here, onward, step in (
                (z >= k, z + 1 < n_z, -1), (z + k < n_z, z >= 1, 1)
            ):
                owner = fs + step * k * n_y
                slot = act_slot(a, owner, tp)
                arrived(slot, act_recv.at[a, owner, tp], here)
                if k < n_z - 1:
                    act_send(
                        a, owner, slot, "fs", fs - step * n_y, jnp.logical_and(here, onward)
                    )
                to_y(a, owner, slot, here)
                to_tp(a, owner, slot, here)
        if n_z >= 3 and k == 1:
            send_weights(soon)
        if n_z >= 3 and k == n_z - 2:
            send_weights(late)
    swap_weights(late)
    for kz in [0] + near_first(n_z):
        for ky in range(1, n_y):
            owner = lax.rem(z + n_z - kz, n_z) * n_y + lax.rem(y + ky, n_y)
            for a in range(2):
                slot = act_slot(a, owner, tp)
                arrived(slot, act_recv.at[a, owner, tp])
                to_tp(a, owner, slot)
    for j in range(1, n_rep):
        half = lax.rem(rep + j, n_rep)
        for k in range(n_fs):
            owner = lax.rem(fs + k, n_fs)
            arrived(w_slot(half, owner), w_recv.at[half, owner])
    for j in range(1, n_tp):
        part = lax.rem(tp + j, n_tp)
        for k in range(n_fs):
            owner = lax.rem(fs + k, n_fs)
            for a in range(2):
                arrived(act_slot(a, owner, part), act_recv.at[a, owner, part])
    out.finish()


def scatter_kernel(
    sizes, d_ref, w_ref, g_ref, x_ref, g_out,
    p, p_in, q, y_in, r, x_in, g_in, g_sum, sends, p_recv, y_recv, x_recv, g_recv, gx_recv,
):
    n_rep, n_fs, n_tp, n_y = sizes
    n_z = n_fs // n_y
    f32, bf16 = jnp.float32, jnp.bfloat16
    rep, fs, tp = (lax.axis_index(axis) for axis in ("rep", "fs", "tp"))
    z, y = fs // n_y, lax.rem(fs, n_y)
    rows, width = x_ref.shape
    depth = g_sum.shape[2]
    enter(n_rep, n_fs, n_tp)
    out = Sender(sends)
    order = near_first(n_fs) + [0]
    zs = near_first(n_z) + [0]

    def columns(part, size):
        return pl.ds(pl.multiple_of(part * size, size), size)

    def g_part(owner, half):
        if depth % 128 == 0:
            return g_ref.at[half, :, columns(owner, depth)]
        return g_ref.at[half, owner]

    for k in order:
        owner = lax.rem(fs + k, n_fs)
        for j in range(1, n_rep):
            peer = lax.rem(rep + j, n_rep)
            out.send(
                g_part(owner, peer), g_in.at[j - 1, owner], g_recv.at[j - 1, owner], "rep", peer
            )
    blocks = [(kz, ky) for ky in list(range(1, n_y)) + [0] for kz in zs]

    def owner_of(kz, ky):
        return lax.rem(z + kz, n_z) * n_y + lax.rem(y + ky, n_y)

    for block in blocks:
        owner = owner_of(*block)
        p[owner] = jnp.dot(
            d_ref[owner], w_ref[: d_ref.shape[2]], preferred_element_type=f32
        ).astype(bf16)
        for j in range(1, n_tp):
            peer = lax.rem(tp + j, n_tp)
            out.send(
                p.at[owner, :, columns(peer, width)],
                p_in.at[j - 1, owner],
                p_recv.at[j - 1, owner],
                "tp",
                peer,
            )

    def pair_sum(owner):
        total = p[owner, :, columns(tp, width)].astype(f32)
        for j in range(n_tp - 1):
            arrived(p_in.at[j, owner], p_recv.at[j, owner])
            total = total + p_in[j, owner].astype(f32)
        return total

    def g_step(k):
        owner = lax.rem(fs + k, n_fs)
        total = g_part(owner, rep)[...].astype(f32)
        for j in range(n_rep - 1):
            arrived(g_in.at[j, owner], g_recv.at[j, owner])
            total = total + g_in[j, owner].astype(f32)
        g_sum[owner] = total.astype(bf16)
        slot = g_out.at[fs, rep]
        if k:
            out.send(g_sum.at[owner], slot, gx_recv.at[rep, fs], "fs", owner)
        else:
            out.local(g_sum.at[owner], slot)
            for j in range(1, n_rep):
                out.send(
                    g_sum.at[owner], slot, gx_recv.at[rep, fs], "rep", lax.rem(rep + j, n_rep)
                )

    for kz, ky in blocks:
        if ky:
            owner = owner_of(kz, ky)
            q[owner] = pair_sum(owner).astype(bf16)
            at = (ky - 1, lax.rem(z + kz, n_z))
            out.send(
                q.at[owner], y_in.at[at], y_recv.at[at], "fs", z * n_y + lax.rem(y + ky, n_y)
            )
    def x_step(kz):
        owner = owner_of(kz, 0)
        z_to = lax.rem(z + kz, n_z)
        total = pair_sum(owner)
        for ky in range(1, n_y):
            at = (ky - 1, z_to)
            arrived(y_in.at[at], y_recv.at[at])
            total = total + y_in[at].astype(f32)
        if kz:
            r[z_to] = total.astype(bf16)
            out.send(r.at[z_to], x_in.at[z], x_recv.at[z], "fs", owner)
        else:
            x_in[z] = total.astype(bf16)

    def g_forward(k):
        if k:
            owner = lax.rem(fs + n_fs - k, n_fs)
            slot = g_out.at[owner, rep]
            arrived(slot, gx_recv.at[rep, owner])
            for j in range(1, n_rep):
                out.send(slot, slot, gx_recv.at[rep, owner], "rep", lax.rem(rep + j, n_rep))

    for i, kz in enumerate(zs):
        for k in order[i * n_y : (i + 1) * n_y]:
            g_step(k)
        x_step(kz)
        if i:
            for k in order[(i - 1) * n_y : i * n_y]:
                g_forward(k)
    for k in order[-n_y:]:
        g_forward(k)
    for kz in near_first(n_z):
        z_from = lax.rem(z + n_z - kz, n_z)
        arrived(x_in.at[z_from], x_recv.at[z_from])
    total = x_in[0].astype(f32)
    for k in range(1, n_z):
        total = total + x_in[k].astype(f32)
    x_ref[...] = total.astype(bf16)
    for j in range(1, n_rep):
        half = lax.rem(rep + j, n_rep)
        for k in range(n_fs):
            owner = lax.rem(fs + k, n_fs)
            arrived(g_out.at[owner, half], gx_recv.at[half, owner])
    out.finish()


VMEM = pl.BlockSpec(memory_space=pltpu.VMEM)
ANY = pl.BlockSpec(memory_space=pl.ANY)
DMA = pltpu.SemaphoreType.DMA


def per_device(n_rep, n_fs, n_tp, x, c, gate_weight, up_weight, down_weight):
    bf16, f32 = jnp.bfloat16, jnp.float32
    n_y = max(k for k in range(1, n_fs + 1) if n_fs % k == 0 and k * k <= n_fs)
    n_z = n_fs // n_y
    tokens, width = x.shape
    depth, hidden_tp = gate_weight.shape
    model = width * n_tp
    units = hidden_tp // n_fs
    step = 16 * n_rep
    rows = -(-3 * units // step) * step
    half = rows // n_rep

    weights = [gate_weight, up_weight, down_weight]
    if units % 16 or depth % 128 or 3 * units <= rows - half:
        blocks = [gate_weight.T, up_weight.T, down_weight]
        blocks = [v.reshape(n_fs, units, depth) for v in blocks]
        blocks.append(jnp.zeros((n_fs, rows - 3 * units, depth), bf16))
        weights = [jnp.concatenate(blocks, axis=1).reshape(n_fs, n_rep, half, depth)]
    aligned = depth % 128 == 0
    w_shape = (n_rep, half, model) if aligned else (n_rep, n_fs, half, depth)
    n_sends = (
        2 * (2 + (2 * n_z - 1) * (n_y - 1) + (2 * n_z - 1) * (n_tp - 1) + 2 * n_z + n_fs * (n_tp - 1) + 1)
        + (n_fs - 1) + n_fs * (n_rep - 1) + 1
    )
    x_all, c_all, w_all = pl.pallas_call(
        functools.partial(gather_kernel, (n_rep, n_fs, n_tp, n_y)),
        out_shape=(
            jax.ShapeDtypeStruct((n_fs, tokens, model), bf16),
            jax.ShapeDtypeStruct((n_fs, tokens, model), bf16),
            jax.ShapeDtypeStruct(w_shape, bf16),
        ),
        in_specs=[VMEM] * (2 + len(weights)),
        out_specs=(ANY,) * 3,
        scratch_shapes=[pltpu.VMEM((n_fs, n_rep, half, depth), bf16), DMA((n_sends,)), DMA((2, n_fs, n_tp)), DMA((n_rep, n_fs))],
        compiler_params=pltpu.CompilerParams(collective_id=0, has_side_effects=True),
    )(x, c, *weights)
    x_all, c_all = (v.reshape(n_fs * tokens, model) for v in (x_all, c_all))
    if not aligned:
        w_all = w_all.transpose(0, 2, 1, 3)
    w_all = w_all.reshape(rows, model)
    w_in, w_down = w_all[: 2 * units], w_all[2 * units : 3 * units]

    last = (((1,), (1,)), ((), ()))
    first = (((0,), (0,)), ((), ()))
    pre = lax.dot_general(x_all, w_in, last, preferred_element_type=f32)
    grad_hidden = lax.dot_general(c_all, w_down, last, preferred_element_type=f32)
    gate_pre, up_pre = pre[:, :units], pre[:, units:]
    sigmoid_gate = jax.nn.sigmoid(gate_pre)
    activated = gate_pre * sigmoid_gate
    hidden = (activated * up_pre).astype(bf16)
    grad_gate = (
        grad_hidden * up_pre * sigmoid_gate * (1.0 + gate_pre * (1.0 - sigmoid_gate))
    ).astype(bf16)
    grad_up = (grad_hidden * activated).astype(bf16)
    grads = jnp.concatenate([grad_gate, grad_up], axis=1)
    g = jnp.concatenate(
        [
            lax.dot_general(grads, x_all, first, preferred_element_type=f32).astype(bf16),
            lax.dot_general(hidden, c_all, first, preferred_element_type=f32).astype(bf16),
            jnp.zeros((rows - 3 * units, model), bf16),
        ],
        axis=0,
    )
    g = g.reshape(w_shape if aligned else (n_rep, half, n_fs, depth))
    if not aligned:
        g = g.transpose(0, 2, 1, 3)
    n_sends = n_fs * (n_tp - 1) + 2 * n_fs * (n_rep - 1) + 3 * n_fs
    grad_inputs, dw = pl.pallas_call(
        functools.partial(scatter_kernel, (n_rep, n_fs, n_tp, n_y)),
        out_shape=(
            jax.ShapeDtypeStruct((tokens, width), bf16),
            jax.ShapeDtypeStruct((n_fs, n_rep, half, depth), bf16),
        ),
        in_specs=[VMEM] * 3,
        out_specs=(VMEM, ANY),
        scratch_shapes=[
            pltpu.VMEM((n_fs, tokens, model), bf16),
            pltpu.VMEM((n_tp - 1, n_fs, tokens, width), bf16),
            pltpu.VMEM((n_fs, tokens, width), bf16),
            pltpu.VMEM((n_y - 1, n_z, tokens, width), bf16),
            pltpu.VMEM((n_z, tokens, width), bf16),
            pltpu.VMEM((n_z, tokens, width), bf16),
            pltpu.VMEM((n_rep - 1, n_fs, half, depth), bf16),
            pltpu.VMEM((n_fs, half, depth), bf16),
            DMA((n_sends,)),
            DMA((n_tp - 1, n_fs)),
            DMA((n_y - 1, n_z)),
            DMA((n_z,)),
            DMA((n_rep - 1, n_fs)),
            DMA((n_rep, n_fs)),
        ],
        compiler_params=pltpu.CompilerParams(
            collective_id=1, has_side_effects=True, vmem_limit_bytes=60 * 2**20
        ),
    )(grads.reshape(n_fs, tokens, 2 * units), w_all, g)
    dw = dw.reshape(n_fs, rows, depth)
    gate_grads, up_grads, down_grads = (
        dw[:, i * units : (i + 1) * units].reshape(hidden_tp, depth) for i in range(3)
    )
    return (
        grad_inputs,
        gate_grads.T.astype(f32),
        up_grads.T.astype(f32),
        down_grads.astype(f32),
    )


def solution(mesh):
    n_rep, n_fs, n_tp = (mesh.shape[axis] for axis in ("rep", "fs", "tp"))
    placed = (
        P(("rep", "fs"), "tp"),
        P(("rep", "fs"), "tp"),
        P("fs", "tp"),
        P("fs", "tp"),
        P("tp", "fs"),
    )
    return jax.shard_map(
        functools.partial(per_device, n_rep, n_fs, n_tp),
        mesh=mesh,
        in_specs=placed,
        out_specs=(P(("rep", "fs"), "tp"), P("fs", "tp"), P("fs", "tp"), P("tp", "fs")),
        check_vma=False,
    )
```
